32 devices in a mesh: fs: 16 (over z, y, x), tp: 2 (over core).
Axes of the slice: x: 2, y: 2, z: 4, core: 2. Of those that a mesh axis runs over, the one named last changes fastest.
Arguments:
- tokens: bfloat16 [6144, 2048], P('fs'), may hold values from -6 to 6
- mixer_norm_gain: float32 [2048], replicated, may hold values from 0.1 to 1.9
- outer_gate_weight: bfloat16 [2048, 2048], P('fs', 'tp'), may hold values from -0.125 to 0.125
- inner_gate_weight: bfloat16 [2048, 2048], P('fs', 'tp'), may hold values from -0.125 to 0.125
- value_projection_weight: bfloat16 [2048, 2048], P('fs', 'tp'), may hold values from -0.125 to 0.125
- filter_taps_weight: float32 [3, 2048], replicated, may hold values from -3 to 3
- mixer_output_weight: bfloat16 [2048, 2048], P('tp', 'fs'), may hold values from -0.125 to 0.125
- feedforward_norm_gain: float32 [2048], replicated, may hold values from 0.1 to 1.9
- up_projection_weight: bfloat16 [2048, 8192], P('fs', 'tp'), may hold values from -0.125 to 0.125
- down_projection_weight: bfloat16 [8192, 2048], P('tp', 'fs'), may hold values from -0.0625 to 0.0625
Outputs:
- layer_out: bfloat16 [6144, 2048], P('fs')
The draws below stay inside these ranges and needn't reach their ends.
All inputs are finite; a program needn't handle non-finite values.
Results may differ from the reference program's by a relative error of at most 0.02.
Values may be sent and summed in bfloat16 or wider, within the bound.
No kernel may reach another device: no remote copies, remote signals or barrier semaphores. Data moves between devices by JAX's collectives and lax.ppermute only.
A program may use at most 128 MiB of HBM per device.

```python
import jax
import jax.numpy as jnp
from jax import lax

MODEL_WIDTH = 2048
MIXER_CHANNELS = 2048
FF = 8192
CONV = 3
TOK_DEV = 384
TOKENS = 6144
N_FS = 16
N_TP = 2


def shard_levels(rng, shape, cuts, smallest, largest):
    level = 1.0
    for axis_at, shards_of in cuts:
        steps = jax.random.uniform(jax.random.fold_in(jax.random.fold_in(rng, 6), axis_at), (shards_of,), jnp.float32, smallest / len(cuts), largest / len(cuts))
        level = level * jnp.repeat(jnp.exp(steps), shape[axis_at] // shards_of).reshape((-1,) + (1,) * (len(shape) - 1 - axis_at))
    return level


def gaussian(stream_key, extent, spread, bound, shards=(), held_as=jnp.bfloat16):
    factor_of = shard_levels(stream_key, extent, shards, -0.22, 0.18) if shards else 1.0
    array = jax.random.normal(stream_key, extent, jnp.float32) * spread * factor_of
    return jnp.minimum(jnp.maximum(array, -bound), bound).astype(held_as)


def setup_inputs(seed: int = 0) -> dict:
    arg_keys = jax.random.split(jax.random.key(seed), 11)
    tokens = gaussian(arg_keys[0], (TOKENS, MODEL_WIDTH), 1.0, 6.0, ((0, 16),))
    mixer_norm_gain = jnp.clip(1.0 + 0.18 * jax.random.normal(arg_keys[1], (MODEL_WIDTH,), jnp.float32), 0.1, 1.9)
    outer_gate_weight = gaussian(arg_keys[2], (MODEL_WIDTH, MIXER_CHANNELS), MODEL_WIDTH ** -0.5, 0.125, ((0, 16), (1, 2)))
    inner_gate_weight = gaussian(arg_keys[3], (MODEL_WIDTH, MIXER_CHANNELS), MODEL_WIDTH ** -0.5, 0.125, ((0, 16), (1, 2)))
    value_projection_weight = gaussian(arg_keys[4], (MODEL_WIDTH, MIXER_CHANNELS), MODEL_WIDTH ** -0.5, 0.125, ((0, 16), (1, 2)))
    filter_taps_weight = gaussian(arg_keys[5], (CONV, MIXER_CHANNELS), 0.577, 3.0, (), jnp.float32)
    mixer_output_weight = gaussian(arg_keys[6], (MIXER_CHANNELS, MODEL_WIDTH), MIXER_CHANNELS ** -0.5, 0.125, ((0, 2), (1, 16)))
    feedforward_norm_gain = jnp.clip(1.0 + 0.18 * jax.random.normal(arg_keys[7], (MODEL_WIDTH,), jnp.float32), 0.1, 1.9)
    up_projection_weight = gaussian(arg_keys[8], (MODEL_WIDTH, FF), MODEL_WIDTH ** -0.5, 0.125, ((0, 16), (1, 2)))
    down_projection_weight = gaussian(arg_keys[9], (FF, MODEL_WIDTH), FF ** -0.5, 0.0625, ((0, 2), (1, 16)))
    return {"tokens": tokens, "mixer_norm_gain": mixer_norm_gain, "outer_gate_weight": outer_gate_weight, "inner_gate_weight": inner_gate_weight, "value_projection_weight": value_projection_weight, "filter_taps_weight": filter_taps_weight, "mixer_output_weight": mixer_output_weight, "feedforward_norm_gain": feedforward_norm_gain, "up_projection_weight": up_projection_weight, "down_projection_weight": down_projection_weight}


def rms_norm(rows, gain):
    floats = rows.astype(jnp.float32)
    scale = lax.rsqrt(lax.optimization_barrier(jnp.mean(floats * floats, axis=-1, keepdims=True)) + 1e-06)
    return (floats * scale * gain).astype(jnp.bfloat16)

def causal_mix(inner_product_rows, taps):
    length = inner_product_rows.shape[0]
    width = taps.shape[0]
    padded = jnp.pad(inner_product_rows, ((width - 1, 0), (0, 0)))
    total = jnp.zeros_like(inner_product_rows)
    for offset in range(width):
        total = total + taps[offset] * padded[offset:offset + length]
    return total

def grouped_sum(left, right, groups):
    count = left.shape[0]
    part = left.shape[1] // groups
    lhs = left.reshape(count, groups, part).astype(jnp.float32)
    rhs = right.reshape(groups, part, right.shape[1]).astype(jnp.float32)
    partial_value = jnp.einsum('rgk,gkd->grd', lhs, rhs).astype(jnp.bfloat16)
    partial_value = lax.optimization_barrier(partial_value).astype(jnp.float32)
    return lax.optimization_barrier(jnp.sum(partial_value, axis=0))

def reference(tokens, mixer_norm_gain, outer_gate_weight, inner_gate_weight, value_projection_weight, filter_taps_weight, mixer_output_weight, feedforward_norm_gain, up_projection_weight, down_projection_weight):

    def one_sequence(rows):
        first_normed_rows = rms_norm(rows, mixer_norm_gain)
        outer_gate_rows = jnp.dot(first_normed_rows, outer_gate_weight, preferred_element_type=jnp.float32).astype(jnp.bfloat16)
        inner_gate_rows = jnp.dot(first_normed_rows, inner_gate_weight, preferred_element_type=jnp.float32).astype(jnp.bfloat16)
        value_rows = jnp.dot(first_normed_rows, value_projection_weight, preferred_element_type=jnp.float32).astype(jnp.bfloat16)
        inner_product_rows = inner_gate_rows.astype(jnp.float32) * value_rows.astype(jnp.float32)
        mixed = (outer_gate_rows.astype(jnp.float32) * causal_mix(inner_product_rows, filter_taps_weight)).astype(jnp.bfloat16)
        resid = (rows.astype(jnp.float32) + grouped_sum(mixed, mixer_output_weight, N_TP)).astype(jnp.bfloat16)
        second = rms_norm(resid, feedforward_norm_gain)
        lifted = jnp.maximum(jnp.dot(second, up_projection_weight, preferred_element_type=jnp.float32), 0.0)
        hidden = (lifted * lifted).astype(jnp.bfloat16)
        return (resid.astype(jnp.float32) + grouped_sum(hidden, down_projection_weight, N_TP)).astype(jnp.bfloat16)
    blocks = tokens.reshape(N_FS, TOK_DEV, MODEL_WIDTH)
    return lax.map(one_sequence, blocks).reshape(TOKENS, MODEL_WIDTH)
```

```python
import jax
import jax.numpy as jnp
from jax import lax
from jax.sharding import PartitionSpec as P


def after(value, *others):
    return lax.optimization_barrier((value,) + others)[0]


class Layout:
    def __init__(self, fs_size, tp_size):
        plane = 1
        while plane * plane * 4 <= fs_size and fs_size % (plane * 2) == 0:
            plane *= 2
        self.size, self.plane, self.lines, self.cores = fs_size, plane, fs_size // plane, tp_size
        index = lax.axis_index("fs")
        self.place, self.line = index % plane, index // plane
        self.core = lax.axis_index("tp")

    def in_plane(self, value, mask):
        pairs = [(i, i ^ mask) for i in range(self.size)]
        return lax.ppermute(value, "fs", pairs)

    def along_line(self, value, direction, step):
        if direction > 0:
            senders = range(step - 1, self.lines - 1)
        else:
            senders = range(1, self.lines - step + 1)
        pairs = [
            (i * self.plane + s, (i + direction) * self.plane + s)
            for i in senders
            for s in range(self.plane)
        ]
        return lax.ppermute(value, "fs", pairs)

    def across_cores(self, value, shift):
        pairs = [(s, (s + shift) % self.cores) for s in range(self.cores)]
        return lax.ppermute(value, "tp", pairs)

    def spread(self, weight, axis):
        width = weight.shape[axis] // self.plane
        stacked = None
        for mask in range(self.plane):
            peer = self.place ^ mask
            part = lax.dynamic_slice_in_dim(weight, peer * width, width, axis)
            if mask:
                part = self.in_plane(part, mask)
            if stacked is None:
                stacked = jnp.zeros((self.plane,) + part.shape, part.dtype)
            stacked = lax.dynamic_update_index_in_dim(stacked, part, peer, 0)
        return stacked

    def gather_line(self, piece, ties=None):
        rising, falling = [piece], [piece]
        for step in range(1, self.lines):
            up, down = rising[-1], falling[-1]
            if step == 1 and ties is not None:
                up, down = after(up, ties[0]), after(down, ties[1])
            rising.append(self.along_line(up, 1, step))
            falling.append(self.along_line(down, -1, step))
        pieces = [piece]
        for step in range(1, self.lines):
            pieces.append(
                jnp.where(self.line + step < self.lines, falling[step], rising[self.lines - step])
            )
        return pieces, (rising[-1], falling[-1])

    def gather_rows(self, rows):
        blocks = []
        for mask in range(self.plane):
            block = self.in_plane(rows, mask) if mask else rows
            chunks = [block] + [self.across_cores(block, -j) for j in range(1, self.cores)]
            blocks.extend(chunks)
        return jnp.concatenate(blocks, axis=0)

    def scatter_sum(self, partial):
        width = partial.shape[1]
        parts = partial.reshape(self.plane, self.cores, -1, width)
        total = parts[:, 0].astype(jnp.float32)
        for j in range(1, self.cores):
            total = total + self.across_cores(parts[:, j], j).astype(jnp.float32)
        rounded = total.astype(jnp.bfloat16)
        mine = total[0]
        for mask in range(1, self.plane):
            mine = mine + self.in_plane(rounded[mask], mask).astype(jnp.float32)
        return mine


def normed(floats, gain):
    scale = lax.rsqrt(jnp.mean(floats * floats, axis=-1, keepdims=True) + 1e-06)
    return (floats * scale * gain).astype(jnp.bfloat16)


def rolled(value, start, axis):
    doubled = jnp.concatenate([value, value], axis=axis)
    return lax.dynamic_slice_in_dim(doubled, start, value.shape[axis], axis)


def product(left, right):
    return jnp.dot(left, right, preferred_element_type=jnp.float32)


def side_by_side(stacked):
    count, depth, width = stacked.shape
    return stacked.transpose(1, 0, 2).reshape(depth, count * width)


def on_device(fs_size, tp_size):
    def run(
        tokens,
        mixer_norm_gain,
        outer_gate_weight,
        inner_gate_weight,
        value_projection_weight,
        filter_taps_weight,
        mixer_output_weight,
        feedforward_norm_gain,
        up_projection_weight,
        down_projection_weight,
    ):
        net = Layout(fs_size, tp_size)
        length, model = tokens.shape
        rows = length // net.cores
        span = model // net.lines
        first_column = net.line * span

        mine = lax.dynamic_slice_in_dim(tokens, net.core * rows, rows, 0)
        mine = rolled(mine, first_column, 1).astype(jnp.float32)
        first = normed(mine, rolled(mixer_norm_gain, first_column, 0))

        gates = [
            net.spread(w, 1)
            for w in (outer_gate_weight, inner_gate_weight, value_projection_weight)
        ]
        channels = gates[0].shape[-1]
        gates = jnp.concatenate(gates, axis=-1).reshape(span, -1)
        mixer_out = net.spread(mixer_output_weight, 0)
        first_rows = net.gather_rows(first)
        ups = net.spread(up_projection_weight, 1).reshape(span, -1)
        downs = net.spread(down_projection_weight, 0)

        gate_pieces, gate_ends = net.gather_line(gates)
        out_pieces, out_ends = net.gather_line(mixer_out)
        up_pieces, up_ends = net.gather_line(ups, gate_ends)
        down_pieces, _ = net.gather_line(downs, up_ends)

        projected = product(first_rows, jnp.concatenate(gate_pieces, axis=0)).astype(jnp.bfloat16)
        projected = projected.reshape(net.plane, length, -1).astype(jnp.float32)
        outer = projected[..., :channels]
        inner = projected[..., channels : 2 * channels] * projected[..., 2 * channels :]
        taps = lax.dynamic_slice_in_dim(
            filter_taps_weight,
            (net.core * net.plane + net.place) * channels,
            channels,
            1,
        )
        position = (jnp.arange(length) + net.core * rows) % length
        count = taps.shape[0]
        convolved = taps[count - 1] * inner
        for back in range(1, count):
            shifted = jnp.concatenate([inner[:, length - back :], inner[:, : length - back]], axis=1)
            shifted = jnp.where((position >= back)[None, :, None], shifted, 0.0)
            convolved = convolved + taps[count - 1 - back] * shifted
        mixed = (outer * convolved).astype(jnp.bfloat16).reshape(net.plane * length, channels)

        sums = [
            net.scatter_sum(product(mixed, side_by_side(w)).astype(jnp.bfloat16))
            for w in out_pieces
        ]
        resid = (mine + jnp.concatenate(sums, axis=1)).astype(jnp.bfloat16).astype(jnp.float32)
        second = normed(resid, rolled(feedforward_norm_gain, first_column, 0))
        second_rows = net.gather_rows(second)
        lifted = jnp.maximum(product(second_rows, jnp.concatenate(up_pieces, axis=0)), 0.0)
        hidden = (lifted * lifted).astype(jnp.bfloat16)

        out = jnp.zeros((length, model), jnp.bfloat16)
        for step, w in enumerate(down_pieces):
            total = net.scatter_sum(product(hidden, side_by_side(w)).astype(jnp.bfloat16))
            piece = (resid[:, step * span : (step + 1) * span] + total).astype(jnp.bfloat16)
            column = (net.line + step) % net.lines * span
            for j in range(net.cores):
                chunk = net.across_cores(piece, -j) if j else piece
                row = (net.core + j) % net.cores * rows
                out = lax.dynamic_update_slice(out, chunk, (row, column))
        return out

    return run


def solution(mesh):
    return jax.shard_map(
        on_device(mesh.shape["fs"], mesh.shape["tp"]),
        mesh=mesh,
        in_specs=(
            P("fs", None),
            P(),
            P("fs", "tp"),
            P("fs", "tp"),
            P("fs", "tp"),
            P(),
            P("tp", "fs"),
            P(),
            P("fs", "tp"),
            P("tp", "fs"),
        ),
        out_specs=P("fs", None),
        check_vma=False,
    )
```

```python
import functools

import jax
import jax.numpy as jnp
from jax import lax
from jax.experimental import pallas as pl
from jax.experimental.pallas import tpu as pltpu
from jax.sharding import PartitionSpec as P


def split_axis(fs_size):
    plane = 1
    while plane * plane * 4 <= fs_size and fs_size % (plane * 2) == 0:
        plane *= 2
    return plane, fs_size // plane


def batches_of(lines):
    if lines < 4:
        return [[s] for s in range(lines)]
    return [list(range(lines - 2)), [lines - 2], [lines - 1]]


def stack_kernel(at_ref, *refs):
    *parts, out, sems = refs
    copies = [
        pltpu.make_async_copy(part, out.at[at_ref[i]], sems.at[i]) for i, part in enumerate(parts)
    ]
    for copy in copies:
        copy.start()
    for copy in copies:
        copy.wait()


def stacked_at(parts, at):
    anywhere = pl.BlockSpec(memory_space=pl.ANY)
    return pl.pallas_call(
        stack_kernel,
        out_shape=jax.ShapeDtypeStruct((len(parts),) + parts[0].shape, parts[0].dtype),
        grid_spec=pltpu.PrefetchScalarGridSpec(
            num_scalar_prefetch=1,
            grid=(1,),
            in_specs=[pl.BlockSpec(memory_space=pltpu.VMEM)] * len(parts),
            out_specs=anywhere,
            scratch_shapes=[pltpu.SemaphoreType.DMA((len(parts),))],
        ),
        name="stack_parts",
    )(at, *parts)


def place_kernel(spots, at_ref, *refs):
    *chunks, out, sems = refs
    copies = []
    for n, (index, slot, chunk, rows, first, span) in enumerate(spots):
        row = pl.multiple_of(at_ref[1, chunk] * rows, rows)
        column = pl.multiple_of(at_ref[0, slot] * span, span)
        copies.append(
            pltpu.make_async_copy(
                chunks[index].at[:, pl.ds(first, span)],
                out.at[pl.ds(row, rows), pl.ds(column, span)],
                sems.at[n],
            )
        )
    for copy in copies:
        copy.start()
    for copy in copies:
        copy.wait()


def placed_at(chunks, spots, at, shape):
    anywhere = pl.BlockSpec(memory_space=pl.ANY)
    return pl.pallas_call(
        functools.partial(place_kernel, spots),
        out_shape=jax.ShapeDtypeStruct(shape, chunks[0].dtype),
        grid_spec=pltpu.PrefetchScalarGridSpec(
            num_scalar_prefetch=1,
            grid=(1,),
            in_specs=[pl.BlockSpec(memory_space=pltpu.VMEM)] * len(chunks),
            out_specs=anywhere,
            scratch_shapes=[pltpu.SemaphoreType.DMA((len(spots),))],
        ),
        name="place_pieces",
    )(at, *chunks)


class Net:
    def __init__(self, fs_size, tp_size):
        self.size, self.cores = fs_size, tp_size
        self.plane, self.lines = split_axis(fs_size)
        index = lax.axis_index("fs").astype(jnp.uint32)
        self.place = (index % self.plane).astype(jnp.int32)
        self.line = (index // self.plane).astype(jnp.int32)
        self.core = lax.axis_index("tp")
        reach = range(self.lines)
        self.order = [sorted(reach, key=lambda j: (abs(j - z), j < z)) for z in reach]

    def source(self, slot):
        result = jnp.int32(self.order[0][slot])
        for z in range(1, self.lines):
            result = jnp.where(self.line == z, self.order[z][slot], result)
        return result

    def in_plane(self, value, mask):
        pairs = [(i, i ^ mask) for i in range(self.size)]
        return lax.ppermute(value, "fs", pairs)

    def along_line(self, value, direction, step):
        if direction > 0:
            senders = range(step - 1, self.lines - 1)
        else:
            senders = range(1, self.lines - step + 1)
        pairs = [
            (i * self.plane + s, (i + direction) * self.plane + s)
            for i in senders
            for s in range(self.plane)
        ]
        return lax.ppermute(value, "fs", pairs)

    def across_cores(self, value, shift):
        pairs = [(s, (s + shift) % self.cores) for s in range(self.cores)]
        return lax.ppermute(value, "tp", pairs)

    def spread(self, part_of):
        peers = [self.place ^ mask for mask in range(self.plane)]
        parts = [part_of(peer) for peer in peers]
        parts = [self.in_plane(p, m) if m else p for m, p in enumerate(parts)]
        at = jnp.stack(peers)
        return stacked_at(parts, at)

    def gather_line(self, piece):
        held = {0: piece}
        for direction in (1, -1):
            value = piece
            for step in range(1, self.lines):
                value = self.along_line(value, direction, step)
                held[-direction * step] = value
        slots = [piece]
        for slot in range(1, self.lines):
            offsets = [self.order[z][slot] - z for z in range(self.lines)]
            result = None
            options = sorted(set(offsets))
            kept = dict(zip(options, lax.optimization_barrier([held[o] for o in options])))
            for offset in options:
                where = [z for z in range(self.lines) if offsets[z] == offset]
                if result is None:
                    result = kept[offset]
                    continue
                here = self.line == where[0]
                for z in where[1:]:
                    here = here | (self.line == z)
                result = jnp.where(here, kept[offset], result)
            slots.append(lax.optimization_barrier(result))
        return slots

    def gather_rows(self, rows):
        blocks = []
        for mask in range(self.plane):
            block = self.in_plane(rows, mask) if mask else rows
            blocks.append(block)
            for j in range(1, self.cores):
                blocks.append(self.across_cores(block, -j))
        return jnp.concatenate(blocks, axis=0)

    def scatter_sum(self, partial):
        parts = partial.reshape(self.plane, self.cores, -1, partial.shape[1])
        total = parts[:, 0].astype(jnp.float32)
        for j in range(1, self.cores):
            total = total + self.across_cores(parts[:, j], j).astype(jnp.float32)
        rounded = total.astype(jnp.bfloat16)
        mine = total[0]
        for mask in range(1, self.plane):
            mine = mine + self.in_plane(rounded[mask], mask).astype(jnp.float32)
        return mine


def normed(floats, gain):
    scale = lax.rsqrt(jnp.mean(floats * floats, axis=-1, keepdims=True) + 1e-06)
    return (floats * scale * gain).astype(jnp.bfloat16)


def product(left, right):
    return jnp.dot(left, right, preferred_element_type=jnp.float32)


def side_by_side(stacked):
    return jnp.concatenate([stacked[s] for s in range(stacked.shape[0])], axis=-1)


def on_device(fs_size, tp_size):
    def run(
        tokens,
        mixer_norm_gain,
        outer_gate_weight,
        inner_gate_weight,
        value_projection_weight,
        filter_taps_weight,
        mixer_output_weight,
        feedforward_norm_gain,
        up_projection_weight,
        down_projection_weight,
    ):
        net = Net(fs_size, tp_size)
        plane, lines, cores = net.plane, net.lines, net.cores
        length, model = tokens.shape
        rows = length // cores
        span = model // lines
        deep = span // plane
        channels = outer_gate_weight.shape[1] // plane
        units = up_projection_weight.shape[1] // plane
        sources = [net.source(slot) for slot in range(lines)]

        def columns(weight, peer, width):
            return lax.dynamic_slice_in_dim(weight, peer * width, width, 1)

        def part_a(peer):
            return jnp.concatenate(
                [columns(w, peer, channels) for w in (inner_gate_weight, value_projection_weight)],
                axis=1,
            )

        def part_b(peer):
            folded = lax.dynamic_slice_in_dim(mixer_output_weight, peer * channels, channels, 0)
            folded = [folded[i : i + deep] for i in range(0, channels, deep)]
            return jnp.concatenate([columns(outer_gate_weight, peer, channels)] + folded, axis=1)

        def reordered(value, axis):
            blocks = [lax.dynamic_slice_in_dim(value, s * span, span, axis) for s in sources]
            return jnp.concatenate(blocks, axis=axis)

        gates_a = net.spread(part_a).reshape(span, -1)
        gates_b = net.spread(part_b).reshape(span, -1)

        mine = lax.dynamic_slice_in_dim(tokens, net.core * rows, rows, 0)
        mine = reordered(mine, 1).astype(jnp.float32)
        first = normed(mine, reordered(mixer_norm_gain, 0))
        first_rows = net.gather_rows(first)

        ups = net.spread(lambda peer: columns(up_projection_weight, peer, units))
        downs = net.spread(
            lambda peer: lax.dynamic_slice_in_dim(down_projection_weight, peer * units, units, 0),
        )

        slots_a = net.gather_line(gates_a)
        slots_b = net.gather_line(gates_b)
        slots_u = net.gather_line(ups.reshape(span, -1))
        slots_d = net.gather_line(downs)

        joined = product(first_rows, jnp.concatenate(slots_a, axis=0)).astype(jnp.bfloat16)
        joined = joined.reshape(plane, length, -1).astype(jnp.float32)
        inner = joined[..., :channels] * joined[..., channels:]
        outer = product(first_rows, jnp.concatenate([b[:, :channels] for b in slots_b], axis=0))
        outer = outer.astype(jnp.bfloat16).reshape(plane, length, -1).astype(jnp.float32)
        first_channel = (net.core * plane + net.place) * channels
        taps = lax.dynamic_slice_in_dim(filter_taps_weight, first_channel, channels, 1)
        position = (jnp.arange(length) + net.core * rows) % length
        count = taps.shape[0]
        convolved = taps[count - 1] * inner
        for back in range(1, count):
            shifted = jnp.concatenate([inner[:, length - back :], inner[:, : length - back]], axis=1)
            shifted = jnp.where((position >= back)[None, :, None], shifted, 0.0)
            convolved = convolved + taps[count - 1 - back] * shifted
        mixed = (outer * convolved).astype(jnp.bfloat16).reshape(plane * length, channels)

        def unfolded(b):
            stacked = b.reshape(plane, deep, -1)
            pieces = [stacked[..., i : i + deep] for i in range(channels, stacked.shape[-1], deep)]
            return side_by_side(jnp.concatenate(pieces, axis=1))

        sums = []
        for half in range(2):
            group = slots_b[half * lines // 2 : (half + 1) * lines // 2]
            weight = jnp.concatenate([unfolded(b) for b in group], axis=1)
            sums.append(net.scatter_sum(product(mixed, weight).astype(jnp.bfloat16)))
        resid = (mine + jnp.concatenate(sums, axis=1)).astype(jnp.bfloat16).astype(jnp.float32)
        second = normed(resid, reordered(feedforward_norm_gain, 0))
        second_rows = net.gather_rows(second)

        lifted = jnp.maximum(product(second_rows, jnp.concatenate(slots_u, axis=0)), 0.0)
        hidden = (lifted * lifted).astype(jnp.bfloat16)

        chunks, spots = [], []
        for group in batches_of(lines):
            weight = jnp.concatenate([side_by_side(slots_d[slot]) for slot in group], axis=1)
            partial = product(hidden, lax.optimization_barrier(weight)).astype(jnp.bfloat16)
            total = net.scatter_sum(partial)
            piece = resid[:, group[0] * span : (group[-1] + 1) * span] + total
            piece = piece.astype(jnp.bfloat16)
            for j in range(cores):
                for i, slot in enumerate(group):
                    spots.append((len(chunks), slot, j, rows, i * span, span))
                chunks.append(net.across_cores(piece, -j) if j else piece)

        count = max(lines, cores)
        holders = [(net.core + j) % cores for j in range(cores)]
        at = [jnp.stack(v + v[:1] * (count - len(v))) for v in (sources, holders)]
        return placed_at(chunks, spots, jnp.stack(at), (length, model))

    return run


def solution(mesh):
    fs_size, tp_size = mesh.shape["fs"], mesh.shape["tp"]
    return jax.shard_map(
        on_device(fs_size, tp_size),
        mesh=mesh,
        in_specs=(
            P("fs", None),
            P(),
            P("fs", "tp"),
            P("fs", "tp"),
            P("fs", "tp"),
            P(),
            P("tp", "fs"),
            P(),
            P("fs", "tp"),
            P("tp", "fs"),
        ),
        out_specs=P("fs", None),
        check_vma=False,
    )
```
